32 devices in a mesh: grp: 2 (over y), fs: 4 (over z), tp: 4 (over x, core).
Axes of the slice: x: 2, y: 2, z: 4, core: 2. Of those that a mesh axis runs over, the one named last changes fastest.
Arguments:
- tokens: bfloat16 [8192, 2048], P(('grp', 'fs', 'tp')), parts along dimension 0, may hold values from -6 to 6
- norm_gains: float32 [4, 2048], replicated, may hold values from 0.1 to 1.9
- query_weight: bfloat16 [2048, 2048], P('fs', 'tp'), may hold values from -0.125 to 0.125
- key_weight: bfloat16 [2048, 2048], P('fs', 'tp'), may hold values from -0.125 to 0.125
- value_weight: bfloat16 [2048, 4096], P('fs', 'tp'), may hold values from -0.125 to 0.125
- swish_weight: bfloat16 [2048, 4096], P('fs', 'tp'), may hold values from -0.125 to 0.125
- mixer_output: bfloat16 [4096, 2048], P('tp', 'fs'), may hold values from -0.09375 to 0.09375
- gate_weight: bfloat16 [2048, 3072], P('fs', 'tp'), may hold values from -0.125 to 0.125
- up_weight: bfloat16 [2048, 3072], P('fs', 'tp'), may hold values from -0.125 to 0.125
- down_weight: bfloat16 [3072, 2048], P('tp', 'fs'), may hold values from -0.109375 to 0.109375
Outputs:
- layer_output: bfloat16 [8192, 2048], P(('grp', 'fs', 'tp')), parts along dimension 0
The draws below stay inside these ranges and needn't reach their ends.
There are 2 independent parts, one for each index of `grp`. The reference program is written for one: setup_inputs(seed, part) draws one part's arguments, and reference() takes and returns one part's arrays. A program takes and returns all parts, laid end to end along the dimension named above; an argument that names none is the same for every part. Nothing has to cross between parts.
All inputs are finite; a program needn't handle non-finite values.
Results may differ from the reference program's by a relative error of at most 0.02.
Values may be sent and summed in bfloat16 or wider, within the bound.
No kernel may reach another device: no remote copies, remote signals or barrier semaphores. Data moves between devices by JAX's collectives and lax.ppermute only.
A program may use at most 128 MiB of HBM per device.

```python
import jax
import jax.numpy as jnp
from jax import lax

D = 2048
H = 8
QK = 256
VD = 512
FF = 3072
BLOCK = 128
SEQ = 1024
TOKENS = 4096
N_TP = 4


def levels(own_key, shape, pieces, low, top_value):
    level, own = 1.0, jax.random.fold_in(own_key, 6)
    for dim, parts in pieces:
        draws = jnp.exp(jax.random.uniform(jax.random.fold_in(own, dim), (parts,), jnp.float32, low / len(pieces), top_value / len(pieces)))
        level = level * jnp.repeat(draws, shape[dim] // parts).reshape([-1 if axis == dim else 1 for axis in range(len(shape))])
    return level


def noise(key, extent, deviation, most, split=(), kind=jnp.bfloat16):
    level = levels(key, extent, split, -0.22, 0.18) if split else 1.0
    array = jax.random.normal(key, extent, jnp.float32) * deviation * level
    return jnp.minimum(jnp.maximum(array, -most), most).astype(kind)


def setup_inputs(seed: int = 0, part: int = 0) -> dict:
    key_of = jax.random.split(jax.random.key(seed), 11)
    part_splits = jax.random.split(jax.random.fold_in(key_of[10], part), 11)
    tokens = noise(part_splits[0], (TOKENS, D), 1.0, 6.0, ((0, 16),))
    norm_gains = jnp.clip(1.0 + 0.18 * jax.random.normal(key_of[1], (4, D), jnp.float32), 0.1, 1.9)
    query_weight = noise(key_of[2], (D, H * QK), D ** -0.5, 0.125, ((0, 4), (1, 4)))
    key_weight = noise(key_of[3], (D, H * QK), D ** -0.5, 0.125, ((0, 4), (1, 4)))
    value_weight = noise(key_of[4], (D, H * VD), D ** -0.5, 0.125, ((0, 4), (1, 4)))
    swish_weight = noise(key_of[5], (D, H * VD), D ** -0.5, 0.125, ((0, 4), (1, 4)))
    mixer_output = noise(key_of[6], (H * VD, D), (H * VD) ** -0.5, 0.09375, ((0, 4), (1, 4)))
    gate_weight = noise(key_of[7], (D, FF), D ** -0.5, 0.125, ((0, 4), (1, 4)))
    up_weight = noise(key_of[8], (D, FF), D ** -0.5, 0.125, ((0, 4), (1, 4)))
    down_weight = noise(key_of[9], (FF, D), FF ** -0.5, 0.109375, ((0, 4), (1, 4)))
    return dict(tokens=tokens, norm_gains=norm_gains, query_weight=query_weight, key_weight=key_weight, value_weight=value_weight, swish_weight=swish_weight, mixer_output=mixer_output, gate_weight=gate_weight, up_weight=up_weight, down_weight=down_weight)


norm_epsilon = 1e-06
group_epsilon = 0.01

def rms_scale(matrix, gain):
    return matrix * lax.rsqrt(lax.optimization_barrier(jnp.mean(matrix * matrix, axis=-1, keepdims=True)) + norm_epsilon) * gain

def rotate_halves(head_tensors, cosine_table, sine_table):
    half_width = head_tensors.shape[-1] // 2
    lower_half = head_tensors[..., :half_width]
    upper_half = head_tensors[..., half_width:]
    return jnp.concatenate([lower_half * cosine_table - upper_half * sine_table, lower_half * sine_table + upper_half * cosine_table], axis=-1)

def decayed_sum(queries, key_rows, value_rows, log_decay):
    query_expanded = queries.astype(jnp.float32)
    key_expanded = key_rows.astype(jnp.float32)
    value_wide = value_rows.astype(jnp.float32)
    retention_scores = jnp.einsum('fzy,czy->zfc', query_expanded, key_expanded)
    offsets = jnp.arange(queries.shape[0], dtype=jnp.float32)
    distance = offsets[:, None] - offsets[None, :]
    weights = jnp.where(distance >= 0, jnp.exp(log_decay[:, None, None] * jnp.maximum(distance, 0.0)), 0.0)
    return jnp.einsum('hnm,mhe->nhe', retention_scores * weights, value_wide)

def grouped_product(active, weight):
    group_width = active.shape[1] // N_TP
    running = jnp.zeros((active.shape[0], weight.shape[1]), jnp.float32)
    for group_index in range(N_TP):
        lower = group_index * group_width
        product = jnp.dot(active[:, lower:lower + group_width], weight[lower:lower + group_width], preferred_element_type=jnp.float32)
        rounded = lax.optimization_barrier(product.astype(jnp.bfloat16))
        running = running + rounded.astype(jnp.float32)
    return running

def reference(tokens, norm_gains, query_weight, key_weight, value_weight, swish_weight, mixer_output, gate_weight, up_weight, down_weight):
    residual = tokens.astype(jnp.float32)
    normed = rms_scale(residual, norm_gains[0]).astype(jnp.bfloat16)
    raw_query = jnp.dot(normed, query_weight, preferred_element_type=jnp.float32)
    raw_keys = jnp.dot(normed, key_weight, preferred_element_type=jnp.float32)
    raw_values = jnp.dot(normed, value_weight, preferred_element_type=jnp.float32)
    raw_swish = jnp.dot(normed, swish_weight, preferred_element_type=jnp.float32)
    seq_count = tokens.shape[0] // SEQ
    positions = jnp.arange(SEQ, dtype=jnp.float32)
    frequency = 10000.0 ** (-jnp.linspace(0.0, 1.0, QK // 2, dtype=jnp.float32))
    angles = positions[:, None] * frequency[None, :]
    cosine_table = jnp.cos(angles)[:, None, :]
    sine_table = jnp.sin(angles)[:, None, :]
    queries = rotate_halves(raw_query.reshape(seq_count, SEQ, H, QK), cosine_table, sine_table).astype(jnp.bfloat16)
    key_rows = (rotate_halves(raw_keys.reshape(seq_count, SEQ, H, QK), cosine_table, sine_table) * QK ** (-0.5)).astype(jnp.bfloat16)
    value_rows = raw_values.reshape(seq_count, SEQ, H, VD).astype(jnp.bfloat16)
    head_index = jnp.arange(H, dtype=jnp.float32)
    log_decay = -(4.0 / BLOCK) * (BLOCK / (32.0 * SEQ)) ** (head_index / (H - 1))
    retained = lax.map(lambda triple: decayed_sum(triple[0], triple[1], triple[2], log_decay), (queries, key_rows, value_rows))
    centred = retained - lax.optimization_barrier(jnp.mean(retained, axis=-1, keepdims=True))
    normalized = centred * lax.rsqrt(lax.optimization_barrier(jnp.mean(centred * centred, axis=-1, keepdims=True)) + group_epsilon)
    gated_rows = (jax.nn.silu(raw_swish) * normalized.reshape(tokens.shape[0], H * VD)).astype(jnp.bfloat16)
    mixer_total = grouped_product(gated_rows, mixer_output)
    after_mixer = residual + rms_scale(mixer_total, norm_gains[1])
    widened = rms_scale(after_mixer, norm_gains[2]).astype(jnp.bfloat16)
    gate_sum = jnp.dot(widened, gate_weight, preferred_element_type=jnp.float32)
    up_sum = jnp.dot(widened, up_weight, preferred_element_type=jnp.float32)
    hidden = (jax.nn.silu(gate_sum) * up_sum).astype(jnp.bfloat16)
    channel = grouped_product(hidden, down_weight)
    return (after_mixer + rms_scale(channel, norm_gains[3])).astype(jnp.bfloat16)
```

```python
import jax
import jax.numpy as jnp
import numpy as np
from jax import lax
from jax.experimental import pallas as pl
from jax.experimental.pallas import tpu as pltpu
from jax.sharding import PartitionSpec as P

H = 8
QK = 256
BLOCK = 128

norm_epsilon = 1e-06
group_epsilon = 0.01


def rms_scale(matrix, gain):
    return (
        matrix * lax.rsqrt(jnp.mean(matrix * matrix, axis=-1, keepdims=True) + norm_epsilon) * gain
    )


def after(value, *earlier):
    return lax.optimization_barrier((value, *earlier))[0]


def folded_ring(size):
    return list(range(0, size, 2)) + list(range(1, size, 2))[::-1]


def retention_kernel(
    place, lam, cosine, sine, query, key, value, swish, gated, state, *, rows, scale
):
    head = pl.program_id(0)
    block = pl.program_id(1)
    rate = lam[head]

    @pl.when(block == 0)
    def _():
        state[...] = jnp.zeros_like(state)

    cos = cosine[...]
    sin = sine[...]
    half = cos.shape[-1]

    def rotate(raw):
        low, high = raw[:, :half], raw[:, half:]
        return jnp.concatenate([low * cos - high * sin, low * sin + high * cos], axis=-1)

    queries = rotate(query[...]).astype(jnp.bfloat16)
    keys = (rotate(key[...]) * scale).astype(jnp.bfloat16)
    values = value[...]
    row = lax.broadcasted_iota(jnp.int32, (rows, rows), 0)
    column = lax.broadcasted_iota(jnp.int32, (rows, rows), 1)
    distance = (row - column).astype(jnp.float32)
    within = jnp.where(distance >= 0, jnp.exp(rate * jnp.maximum(distance, 0.0)), 0.0)
    scores = lax.dot_general(
        queries, keys, (((1,), (1,)), ((), ())), preferred_element_type=jnp.float32
    )
    local = jnp.dot(
        (scores * within).astype(jnp.bfloat16), values, preferred_element_type=jnp.float32
    )
    offset = lax.broadcasted_iota(jnp.int32, (rows, 1), 0).astype(jnp.float32)
    carried = jnp.dot(
        queries, state[...].astype(jnp.bfloat16), preferred_element_type=jnp.float32
    )
    retained = local + carried * jnp.exp(rate * (offset + 1.0))
    faded = (keys.astype(jnp.float32) * jnp.exp(rate * (rows - 1.0 - offset))).astype(jnp.bfloat16)
    whole_fade = jnp.exp(jnp.full((1, 1), rate * rows, jnp.float32))
    state[...] = state[...] * whole_fade + lax.dot_general(
        faded, values, (((0,), (0,)), ((), ())), preferred_element_type=jnp.float32
    )
    centred = retained - jnp.mean(retained, axis=-1, keepdims=True)
    normalized = centred * lax.rsqrt(
        jnp.mean(centred * centred, axis=-1, keepdims=True) + group_epsilon
    )
    gate = swish[...]
    gated[...] = (gate / (1.0 + jnp.exp(-gate)) * normalized).astype(jnp.bfloat16)


def retention(place, lam, cosine, sine, query, key, value, swish, rows):
    length, heads = query.shape[0], query.shape[1] // QK
    width = value.shape[1] // heads
    blocks = length // rows

    def at_row(h, b, place, lam):
        return (place[b], h)

    def at_block(h, b, place, lam):
        return (b, 0)

    return pl.pallas_call(
        lambda *refs: retention_kernel(*refs, rows=rows, scale=QK ** (-0.5)),
        grid_spec=pltpu.PrefetchScalarGridSpec(
            num_scalar_prefetch=2,
            grid=(heads, blocks),
            in_specs=[
                pl.BlockSpec((rows, QK // 2), at_block),
                pl.BlockSpec((rows, QK // 2), at_block),
                pl.BlockSpec((rows, QK), at_row),
                pl.BlockSpec((rows, QK), at_row),
                pl.BlockSpec((rows, width), at_row),
                pl.BlockSpec((rows, width), at_row),
            ],
            out_specs=pl.BlockSpec((rows, width), at_row),
            scratch_shapes=[pltpu.VMEM((QK, width), jnp.float32)],
        ),
        out_shape=jax.ShapeDtypeStruct((length, heads * width), jnp.bfloat16),
        cost_estimate=pl.CostEstimate(
            flops=2 * length * heads * (rows * (QK + width) + 2 * QK * width),
            bytes_accessed=length * heads * (8 * QK + 8 * width),
            transcendentals=length * heads * (rows + width),
        ),
        name="retention",
    )(place, lam, cosine, sine, query, key, value, swish)


def solution(mesh):
    groups, line, team = mesh.shape["grp"], mesh.shape["fs"], mesh.shape["tp"]
    ring = folded_ring(line)
    ring_pairs = [(ring[i], ring[(i + 1) % line]) for i in range(line)]
    before = {b: a for a, b in ring_pairs}
    source = np.zeros((line, line), np.int32)
    for z in range(line):
        source[z, 0] = z
        for j in range(1, line):
            source[z, j] = before[source[z, j - 1]]
    arrival = np.argsort(source, axis=1).astype(np.int32)
    swap_pairs = [(0, 1), (1, 0)]
    bits = [1 << b for b in range(team.bit_length() - 1)]
    bits = [bits[0]] + bits[:0:-1]
    slot = np.zeros(team, np.int32)
    for difference in range(team):
        for i, bit in enumerate(bits):
            if difference & bit:
                slot[difference] += 1 << (len(bits) - 1 - i)

    def exchange(value, bit):
        return lax.ppermute(value, "tp", [(i, i ^ bit) for i in range(team)])

    def gather_rows(own):
        for bit in bits[::-1]:
            own = jnp.concatenate([own, exchange(own, bit)], axis=0)
        return own

    def scatter_sum(partial):
        total = partial
        for bit in bits:
            rows = total.shape[0] // 2
            away = total[rows:].astype(jnp.bfloat16)
            total = total[:rows].astype(jnp.float32) + exchange(away, bit).astype(jnp.float32)
        return total

    def per_device(
        tokens,
        norm_gains,
        query_weight,
        key_weight,
        value_weight,
        swish_weight,
        mixer_output,
        gate_weight,
        up_weight,
        down_weight,
    ):
        g = lax.axis_index("grp")
        z = lax.axis_index("fs")
        t = lax.axis_index("tp")
        width = tokens.shape[1]
        piece = width // (line * groups)
        order = [jnp.asarray(source)[z, j] for j in range(line)]
        sides = [g, 1 - g] if groups == 2 else [0]

        def to_ring(array):
            return jnp.concatenate(
                [
                    lax.dynamic_slice_in_dim(array, (s * groups + h) * piece, piece, axis=1)
                    for s in order
                    for h in sides
                ],
                axis=1,
            )

        def from_ring(array):
            places = [jnp.asarray(arrival)[z, s] for s in range(line)]
            return jnp.concatenate(
                [
                    lax.dynamic_slice_in_dim(
                        array, (p * groups + (h ^ g)) * piece, piece, axis=1
                    )
                    for p in places
                    for h in range(groups)
                ],
                axis=1,
            )

        def halves(shard, axis):
            size = shard.shape[axis] // groups
            return [lax.dynamic_slice_in_dim(shard, h * size, size, axis=axis) for h in sides]

        kinds = dict(
            qk=halves(jnp.concatenate([query_weight, key_weight], axis=1), 0),
            v=halves(value_weight, 0),
            s=halves(swish_weight, 0),
            mo=halves(mixer_output, 1),
            gu=halves(jnp.concatenate([gate_weight, up_weight], axis=1), 0),
            down=halves(down_weight, 1),
        )
        axis_of = dict(qk=0, v=0, s=0, mo=1, gu=0, down=1)
        received = {name: [parts[0]] for name, parts in kinds.items()}
        swapped = {name: parts[1:] for name, parts in kinds.items()}
        last = []
        for pair in (("qk", "v"), ("s", "mo"), ("gu", "down")):
            ends = []
            for step in range(1, line):
                for name in pair:
                    value = received[name][-1]
                    if step == 1 and last:
                        value = after(value, last[0 if name == pair[0] else -1])
                    with jax.named_scope(f"z_{name}_{step}"):
                        value = lax.ppermute(value, "fs", ring_pairs)
                    received[name].append(value)
                    if groups == 2:
                        with jax.named_scope(f"y_{name}_{step}"):
                            swapped[name].append(lax.ppermute(value, "grp", swap_pairs))
                    if step == line - 1:
                        ends.append(value)
            last = ends

        def whole(name):
            blocks = []
            for j in range(line):
                blocks.append(received[name][j])
                if groups == 2:
                    blocks.append(swapped[name][j])
            return jnp.concatenate(blocks, axis=axis_of[name])

        residual = to_ring(tokens).astype(jnp.float32)
        gains = to_ring(norm_gains)
        normed = gather_rows(rms_scale(residual, gains[0]).astype(jnp.bfloat16))
        length = normed.shape[0]
        rows = tokens.shape[0]
        positions = jnp.arange(length, dtype=jnp.float32)
        frequency = 10000.0 ** (-jnp.linspace(0.0, 1.0, QK // 2, dtype=jnp.float32))
        angles = positions[:, None] * frequency[None, :]
        cosine_table = jnp.cos(angles)
        sine_table = jnp.sin(angles)
        heads = query_weight.shape[1] // QK
        place = jnp.asarray(slot)[jnp.arange(team, dtype=jnp.int32) ^ t]
        head_index = (t * heads + jnp.arange(heads)).astype(jnp.float32)
        log_decay = -(4.0 / BLOCK) * (BLOCK / (32.0 * length)) ** (head_index / (H - 1))

        def dot(a, b):
            return jnp.dot(a, b, preferred_element_type=jnp.float32)

        query_key = dot(normed, whole("qk"))
        keys_at = heads * QK
        values = dot(normed, whole("v")).astype(jnp.bfloat16)
        swish = dot(normed, whole("s"))
        gated = retention(
            place,
            log_decay,
            cosine_table,
            sine_table,
            query_key[:, :keys_at],
            query_key[:, keys_at:],
            values,
            swish,
            rows,
        )
        mixer_total = scatter_sum(dot(gated, whole("mo")).astype(jnp.bfloat16))
        after_mixer = residual + rms_scale(mixer_total, gains[1])
        widened = gather_rows(rms_scale(after_mixer, gains[2]).astype(jnp.bfloat16))
        gate_up = dot(widened, whole("gu"))
        units = gate_weight.shape[1]
        hidden = (jax.nn.silu(gate_up[:, :units]) * gate_up[:, units:]).astype(jnp.bfloat16)
        channel = scatter_sum(dot(hidden, whole("down")).astype(jnp.bfloat16))
        result = (after_mixer + rms_scale(channel, gains[3])).astype(jnp.bfloat16)
        return from_ring(result)

    placed = (
        P(("grp", "fs", "tp"), None),
        P(),
        P("fs", "tp"),
        P("fs", "tp"),
        P("fs", "tp"),
        P("fs", "tp"),
        P("tp", "fs"),
        P("fs", "tp"),
        P("fs", "tp"),
        P("tp", "fs"),
    )
    return jax.shard_map(
        per_device,
        mesh=mesh,
        in_specs=placed,
        out_specs=P(("grp", "fs", "tp"), None),
        check_vma=False,
    )
```
